32 devices in a mesh: rep: 8 (over z, y), fs: 2 (over x), tp: 2 (over core).
Axes of the slice: x: 2, y: 2, z: 4, core: 2. Of those that a mesh axis runs over, the one named last changes fastest.
Arguments:
- inputs: bfloat16 [4096, 2048], P(('rep', 'tp'), 'fs'), may hold values from -6 to 6
- pre_act: bfloat16 [4096, 4096], P(('rep', 'fs'), 'tp'), may hold values from -6 to 6
- cotangent: bfloat16 [4096, 2048], P(('rep', 'tp'), 'fs'), may hold values from -6 to 6
- up_weight: bfloat16 [2048, 4096], P('fs', 'tp'), may hold values from -0.125 to 0.125
- down_weight: bfloat16 [4096, 2048], P('tp', 'fs'), may hold values from -0.09375 to 0.09375
Outputs:
- grad_inputs: bfloat16 [4096, 2048], P(('rep', 'tp'), 'fs')
- grad_up: float32 [2048, 4096], P('fs', 'tp')
- grad_down: float32 [4096, 2048], P('tp', 'fs')
The draws below stay inside these ranges and needn't reach their ends.
All inputs are finite; a program needn't handle non-finite values.
Results may differ from the reference program's by a relative error of at most 0.015.
Values may be sent and summed in bfloat16 or wider, within the bound.
A program may use at most 128 MiB of HBM per device.

```python
import jax
import jax.numpy as jnp
from jax import lax

D = 2048
FF = 4096
TOKENS = 4096
N_TP = 2


def raised(array, rng, source, target, parts, factor):
    owner, partner = [(jnp.arange(array.shape[position]) // (array.shape[position] // parts)).reshape([-1 if axis == position else 1 for axis in range(array.ndim)]) for position in (source, target)]
    chosen = jax.random.permutation(rng, parts)[partner]
    strong = (owner == chosen) | (owner == (partner + parts // 2) % parts)
    return jnp.where(strong, factor * array, array)


def block_levels(stream_key, shape, shards, low, top_value):
    def one(dim, blocks):
        heights = jax.random.uniform(jax.random.fold_in(jax.random.fold_in(stream_key, 6), dim), (blocks,), jnp.float32, low / len(shards), top_value / len(shards))
        return jnp.repeat(jnp.exp(heights), shape[dim] // blocks).reshape((-1,) + (1,) * (len(shape) - dim - 1))

    level = one(*shards[0])
    for cut in shards[1:]:
        level = level * one(*cut)
    return level


def bell_draw(key, dims, scale, reach, pieces=(), held_as=jnp.bfloat16):
    values = jax.random.normal(key, dims, jnp.float32) * scale
    if len(pieces) > 0:
        values = block_levels(key, dims, pieces, -0.22, 0.18) * values
    return jnp.clip(values, min=-reach, max=reach).astype(held_as)


def bell_draw_with(rng, shape, spread, limit, split, heavy, dtype=jnp.bfloat16):
    entries = spread * jax.random.normal(rng, shape, jnp.float32)
    if split:
        entries = entries * block_levels(rng, shape, split, -0.22, 0.18)
    return jnp.clip(raised(entries, jax.random.fold_in(rng, 3), *heavy), -limit, limit).astype(dtype)


def setup_inputs(seed: int = 0) -> dict:
    splits = jax.random.split(jax.random.key(seed), 6)
    return {
        "inputs": bell_draw(splits[0], (TOKENS, D), 1.0, 6.0, ((0, 16), (1, 2))),
        "pre_act": bell_draw(splits[1], (TOKENS, FF), 1.0, 6.0, ((0, 16), (1, 2))),
        "cotangent": bell_draw_with(splits[2], (TOKENS, D), 1.0, 6.0, ((0, 16), (1, 2)), (0, 1, 16, 2.0)),
        "up_weight": bell_draw(splits[3], (D, FF), D ** -0.5, 0.125, ((0, 2), (1, 2))),
        "down_weight": bell_draw(splits[4], (FF, D), FF ** -0.5, 0.09375, ((0, 2), (1, 2))),
    }


def reference(inputs, pre_act, cotangent, up_weight, down_weight):
    positive = jnp.maximum(pre_act.astype(jnp.float32), 0.0)
    square = (positive * positive).astype(jnp.bfloat16)
    grad_act = jnp.dot(cotangent, down_weight.T, preferred_element_type=jnp.float32)
    grad_pre = (2.0 * positive * grad_act).astype(jnp.bfloat16)
    factor = TOKENS ** -0.5
    grad_down = jnp.dot(square.T, cotangent, preferred_element_type=jnp.float32) * factor
    grad_up = jnp.dot(inputs.T, grad_pre, preferred_element_type=jnp.float32) * factor
    width = FF // N_TP
    total = jnp.zeros(inputs.shape, jnp.float32)
    for block in range(N_TP):
        partial_sum = jnp.dot(grad_pre[:, block * width:(block + 1) * width],
                              up_weight[:, block * width:(block + 1) * width].T,
                              preferred_element_type=jnp.float32).astype(jnp.bfloat16)
        partial_sum = lax.optimization_barrier(partial_sum)
        total = total + partial_sum.astype(jnp.float32)
    grad_inputs = total.astype(jnp.bfloat16)
    return grad_inputs, grad_up, grad_down
```

```python
import functools

import jax
import jax.numpy as jnp
from jax import lax
from jax.experimental import pallas as pl
from jax.experimental.pallas import tpu as pltpu
from jax.sharding import PartitionSpec as P

MESH = pl.DeviceIdType.MESH
LANES = 128
F32, BF16 = jnp.float32, jnp.bfloat16


def rows_dot(left, right):
    return lax.dot_general(left, right, (((0,), (0,)), ((), ())), preferred_element_type=F32)


def cols_dot(left, right):
    return lax.dot_general(left, right, (((1,), (1,)), ((), ())), preferred_element_type=F32)


def plan(n_rep, width, hidden):
    panels = hidden // LANES
    subs = 2 if width * panels // (4 * n_rep) >= 2 * LANES else 1
    per_panel = 2 * n_rep * subs // panels
    return subs, per_panel, width // per_panel


def kernel(
    n_rep, x_ref, pre_ref, cot_ref, wu_hbm, wd_hbm,
    gi_ref, up_ref, down_ref,
    wu, wd, xg, cg, pre_in, sq, gp, pa_own, pa_out, pa_in, gi_out, gi_in,
    first_d, first_u, rs_d, rs_u,
    w_sem, tp_s, tp_r, pre_s, pre_r, gp_s, gp_r, pa_s, pa_r, gi_s, gi_r,
    rsd_s, rsd_r, rsu_s, rsu_r, agd_s, agd_r, agu_s, agu_r,
):
    half, width = x_ref.shape
    hidden = pre_ref.shape[1]
    panels = hidden // LANES
    subs, per_panel, w = plan(n_rep, width, hidden)
    fine = 2 * n_rep == panels
    rep, fs, tp = lax.axis_index("rep"), lax.axis_index("fs"), lax.axis_index("tp")
    line = n_rep // 2
    row, col = rep // 2, rep % 2
    pos = jnp.where(col == 0, row, n_rep - 1 - row)

    def rep_at(p):
        p = lax.rem(p + n_rep, n_rep)
        return jnp.where(p < line, 2 * p, 2 * (n_rep - 1 - p) + 1)

    nxt, prv = rep_at(pos + 1), rep_at(pos + n_rep - 1)
    goal = ({"rep": nxt}, {"rep": prv})
    other_fs, other_tp = {"fs": 1 - fs}, {"tp": 1 - tp}
    mine_f = pl.ds(pl.multiple_of(fs * half, half), half)
    his_f = pl.ds(pl.multiple_of((1 - fs) * half, half), half)
    mine_t = pl.ds(pl.multiple_of(tp * half, half), half)
    his_t = pl.ds(pl.multiple_of((1 - tp) * half, half), half)

    def remote(src, dst, s, r, dev):
        return pltpu.make_async_remote_copy(
            src_ref=src, dst_ref=dst, send_sem=s, recv_sem=r, device_id=dev,
            device_id_type=MESH)

    load_wd = pltpu.make_async_copy(wd_hbm, wd, w_sem.at[0])
    load_wu = pltpu.make_async_copy(wu_hbm, wu, w_sem.at[1])
    load_wd.start()
    load_wu.start()

    barrier = pltpu.get_barrier_semaphore()
    for dev in (goal[0], goal[1], other_fs, other_tp):
        pl.semaphore_signal(barrier, inc=1, device_id=dev, device_id_type=MESH)
    pl.semaphore_wait(barrier, 4)

    def chunk_of(d, j):
        return lax.rem(pos + (-1 - j if d == 0 else 1 + j) + 2 * n_rep, n_rep)

    def lanes(panel):
        return pl.ds(pl.multiple_of(panel * LANES, LANES), LANES)

    def panel_of(d, j):
        return d * n_rep + chunk_of(d, j)

    def pre_copy(panel):
        return remote(pre_ref.at[:, lanes(panel)], pre_in.at[:, lanes(panel)],
                      pre_s.at[panel], pre_r.at[panel], other_fs)

    def gp_copy(panel):
        return remote(gp.at[mine_f, lanes(panel)], gp.at[mine_f, lanes(panel)],
                      gp_s.at[panel], gp_r.at[panel], other_fs)

    def in_order(body):
        if fine:
            def step(j, _):
                body(panel_of(0, j))
                body(panel_of(1, j))
                return 0
            lax.fori_loop(0, n_rep, step, 0)
        else:
            def step(j, _):
                body(j)
                return 0
            lax.fori_loop(0, panels, step, 0)

    cot_move = remote(cot_ref, cg.at[mine_t, :], tp_s.at[0], tp_r.at[0], other_tp)
    x_move = remote(x_ref, xg.at[mine_t, :], tp_s.at[1], tp_r.at[1], other_tp)
    cot_move.start()
    in_order(lambda panel: pre_copy(panel).start())
    x_move.start()
    cg[mine_t, :] = cot_ref[...]
    xg[mine_t, :] = x_ref[...]

    def square_of(block):
        positive = jnp.maximum(block.astype(F32), 0.0)
        return (positive * positive).astype(BF16)

    def own_square(j, _):
        sq[mine_f, lanes(j)] = square_of(pre_ref[:, lanes(j)])
        return 0
    lax.fori_loop(0, panels, own_square, 0)

    def pre_arrived(panel):
        pre_copy(panel).wait_recv()
        sq[his_f, lanes(panel)] = square_of(pre_in[:, lanes(panel)])

    def gp_arrived(panel):
        gp_copy(panel).wait_recv()

    def prepare(body, j):
        if fine:
            body(panel_of(0, j))
            body(panel_of(1, j))

    def where(d, chunk, sub):
        block = (d * n_rep + chunk) * subs + sub
        return lanes(block // per_panel), pl.ds(
            pl.multiple_of(lax.rem(block, per_panel) * w, w), w)

    def down_at(d, chunk, sub):
        hid, wid = where(d, chunk, sub)
        return down_ref.at[hid, wid]

    def up_at(d, chunk, sub):
        hid, wid = where(d, chunk, sub)
        return up_ref.at[wid, hid]

    def down_block(d, chunk, sub):
        hid, wid = where(d, chunk, sub)
        return rows_dot(sq[:, hid], cg[:, wid])

    def up_block(d, chunk, sub):
        hid, wid = where(d, chunk, sub)
        return rows_dot(xg[:, wid], gp[:, hid])

    def rs_copy(first, slots, s_sem, r_sem, d, sub, s, src=None):
        src = slots.at[d, sub, s - 1] if src is None else src
        return remote(src, slots.at[d, sub, s], s_sem.at[d, sub, s], r_sem.at[d, sub, s],
                      goal[d])

    def ag_copy(at, s_sem, r_sem, d, sub, s):
        chunk = lax.rem(pos + (-s if d == 0 else s) + n_rep, n_rep)
        return remote(at(d, chunk, sub), at(d, chunk, sub), s_sem.at[d, sub, s],
                      r_sem.at[d, sub, s], goal[d])

    streams = [(d, sub) for sub in range(subs) for d in range(2)]

    def rs_open(block, first, slots, s_sem, r_sem):
        for d, sub in streams:
            first[d, sub] = block(d, chunk_of(d, 0), sub).astype(BF16)
            rs_copy(first, slots, s_sem, r_sem, d, sub, 0, first.at[d, sub]).start()

    def rs_step(block, first, slots, s_sem, r_sem, j, d, sub):
        part = block(d, chunk_of(d, j), sub)
        rs_copy(first, slots, s_sem, r_sem, d, sub, j - 1, first.at[d, sub]).wait_recv()
        slots[d, sub, j - 1] = (slots[d, sub, j - 1].astype(F32) + part).astype(BF16)
        rs_copy(first, slots, s_sem, r_sem, d, sub, j).start()

    def rs_close(block, at, first, slots, s_sem, r_sem, as_, ar, d, sub):
        part = block(d, pos, sub)
        last = n_rep - 2
        rs_copy(first, slots, s_sem, r_sem, d, sub, last, first.at[d, sub]).wait_recv()
        at(d, pos, sub)[...] = (slots[d, sub, last].astype(F32) + part).astype(BF16)
        ag_copy(at, as_, ar, d, sub, 0).start()

    def ag_step(at, as_, ar, s, d, sub):
        chunk = lax.rem(pos + (-s if d == 0 else s) + n_rep, n_rep)
        remote(at(d, chunk, sub), at(d, chunk, sub), as_.at[d, sub, s - 1],
               ar.at[d, sub, s - 1], goal[d]).wait_recv()
        ag_copy(at, as_, ar, d, sub, s).start()

    def ag_close(at, as_, ar, d, sub):
        s = n_rep - 1
        chunk = lax.rem(pos + (-s if d == 0 else s) + n_rep, n_rep)
        remote(at(d, chunk, sub), at(d, chunk, sub), as_.at[d, sub, s - 1],
               ar.at[d, sub, s - 1], goal[d]).wait_recv()

    down = (first_d, rs_d, rsd_s, rsd_r)
    up = (first_u, rs_u, rsu_s, rsu_r)

    cot_move.wait_recv()
    if fine:
        prepare(pre_arrived, 0)
    else:
        in_order(pre_arrived)
    rs_open(down_block, *down)

    load_wd.wait()
    piece = min(2 * LANES, hidden)

    def act_step(n, _):
        at = pl.ds(pl.multiple_of(n * piece, piece), piece)
        pa_out[:, at] = cols_dot(cg[his_f, :], wd[at, :]).astype(BF16)
        return 0
    lax.fori_loop(0, hidden // piece, act_step, 0)
    pa_move = remote(pa_out, pa_in, pa_s, pa_r, other_fs)
    pa_move.start()

    def act_own(n, _):
        at = pl.ds(pl.multiple_of(n * piece, piece), piece)
        pa_own[:, at] = cols_dot(cg[mine_f, :], wd[at, :])
        return 0
    lax.fori_loop(0, hidden // piece, act_own, 0)

    def down_step(j, _):
        prepare(pre_arrived, j)
        for d, sub in streams:
            rs_step(down_block, *down, j, d, sub)
        return 0
    lax.fori_loop(1, n_rep - 1, down_step, 0)
    prepare(pre_arrived, n_rep - 1)
    for d, sub in streams:
        rs_close(down_block, down_at, *down, agd_s, agd_r, d, sub)

    pa_move.wait_recv()

    def pre_grad(panel):
        at = lanes(panel)
        positive = jnp.maximum(pre_ref[:, at].astype(F32), 0.0)
        grad = pa_own[:, at] + pa_in[:, at].astype(F32)
        gp[mine_f, at] = (2.0 * positive * grad).astype(BF16)
        gp_copy(panel).start()
    in_order(pre_grad)
    x_move.wait_recv()
    if fine:
        prepare(gp_arrived, 0)
    else:
        in_order(gp_arrived)
    rs_open(up_block, *up)

    def both_step(j, _):
        prepare(gp_arrived, j)
        for d, sub in streams:
            ag_step(down_at, agd_s, agd_r, j, d, sub)
            rs_step(up_block, *up, j, d, sub)
        return 0
    lax.fori_loop(1, n_rep - 1, both_step, 0)
    prepare(gp_arrived, n_rep - 1)
    for d, sub in streams:
        ag_close(down_at, agd_s, agd_r, d, sub)
        rs_close(up_block, up_at, *up, agu_s, agu_r, d, sub)

    load_wu.wait()
    wide = min(2 * LANES, width)

    def input_out(n, _):
        at = pl.ds(pl.multiple_of(n * wide, wide), wide)
        gi_out[:, at] = cols_dot(gp[his_t, :], wu[at, :]).astype(BF16)
        return 0
    lax.fori_loop(0, width // wide, input_out, 0)
    gi_move = remote(gi_out, gi_in, gi_s, gi_r, other_tp)
    gi_move.start()

    def gather_step(j, _):
        for d, sub in streams:
            ag_step(up_at, agu_s, agu_r, j, d, sub)
        return 0
    lax.fori_loop(1, n_rep - 1, gather_step, 0)

    gi_move.wait_recv()

    def input_own(n, _):
        at = pl.ds(pl.multiple_of(n * wide, wide), wide)
        own = cols_dot(gp[mine_t, :], wu[at, :]).astype(BF16).astype(F32)
        gi_ref[:, at] = (own + gi_in[:, at].astype(F32)).astype(BF16)
        return 0
    lax.fori_loop(0, width // wide, input_own, 0)
    for d, sub in streams:
        ag_close(up_at, agu_s, agu_r, d, sub)

    for move in (cot_move, x_move, pa_move, gi_move):
        move.wait_send()

    def sent_panels(j, _):
        pre_copy(j).wait_send()
        gp_copy(j).wait_send()
        return 0
    lax.fori_loop(0, panels, sent_panels, 0)

    def sent_steps(s, _):
        for d, sub in streams:
            rs_copy(*down, d, sub, s, first_d.at[d, sub]).wait_send()
            rs_copy(*up, d, sub, s, first_u.at[d, sub]).wait_send()
            ag_copy(down_at, agd_s, agd_r, d, sub, s).wait_send()
            ag_copy(up_at, agu_s, agu_r, d, sub, s).wait_send()
        return 0
    lax.fori_loop(0, n_rep - 1, sent_steps, 0)


def per_device(n_rep, inputs, pre_act, cotangent, up_weight, down_weight):
    half, width = inputs.shape
    hidden = pre_act.shape[1]
    panels = hidden // LANES
    subs, per_panel, w = plan(n_rep, width, hidden)
    dma = pltpu.SemaphoreType.DMA
    ring = [dma((2, subs, n_rep - 1))] * 2
    vmem = pl.BlockSpec(memory_space=pltpu.VMEM)
    anywhere = pl.BlockSpec(memory_space=pl.ANY)
    grad_inputs, grad_up, grad_down = pl.pallas_call(
        functools.partial(kernel, n_rep),
        name="ffn_backward",
        out_shape=(
            jax.ShapeDtypeStruct((half, width), BF16),
            jax.ShapeDtypeStruct((width, hidden), BF16),
            jax.ShapeDtypeStruct((hidden, width), BF16),
        ),
        in_specs=[vmem, vmem, vmem, anywhere, anywhere],
        out_specs=(vmem, vmem, vmem),
        scratch_shapes=[
            pltpu.VMEM((width, hidden), BF16),
            pltpu.VMEM((hidden, width), BF16),
            pltpu.VMEM((2 * half, width), BF16),
            pltpu.VMEM((2 * half, width), BF16),
            pltpu.VMEM((half, hidden), BF16),
            pltpu.VMEM((2 * half, hidden), BF16),
            pltpu.VMEM((2 * half, hidden), BF16),
            pltpu.VMEM((half, hidden), F32),
            pltpu.VMEM((half, hidden), BF16),
            pltpu.VMEM((half, hidden), BF16),
            pltpu.VMEM((half, width), BF16),
            pltpu.VMEM((half, width), BF16),
            pltpu.VMEM((2, subs, LANES, w), BF16),
            pltpu.VMEM((2, subs, w, LANES), BF16),
            pltpu.VMEM((2, subs, n_rep - 1, LANES, w), BF16),
            pltpu.VMEM((2, subs, n_rep - 1, w, LANES), BF16),
            dma((2,)), dma((2,)), dma((2,)),
            dma((panels,)), dma((panels,)), dma((panels,)), dma((panels,)),
            dma, dma, dma, dma,
            *ring, *ring, *ring, *ring,
        ],
        compiler_params=pltpu.CompilerParams(
            collective_id=0, has_side_effects=True, vmem_limit_bytes=58 * 2**20
        ),
    )(inputs, pre_act, cotangent, up_weight, down_weight)
    factor = (half * n_rep * lax.axis_size("tp")) ** (-0.5)
    return grad_inputs, grad_up.astype(F32) * factor, grad_down.astype(F32) * factor


def solution(mesh):
    assert mesh.shape["fs"] == 2 and mesh.shape["tp"] == 2
    placed = (
        P(("rep", "tp"), "fs"),
        P(("rep", "fs"), "tp"),
        P(("rep", "tp"), "fs"),
        P("fs", "tp"),
        P("tp", "fs"),
    )
    return jax.shard_map(
        functools.partial(per_device, mesh.shape["rep"]),
        mesh=mesh,
        in_specs=placed,
        out_specs=(P(("rep", "tp"), "fs"), P("fs", "tp"), P("tp", "fs")),
        check_vma=False,
    )
```

```python
import functools

import jax
import jax.numpy as jnp
from jax import lax
from jax.experimental import pallas as pl
from jax.experimental.pallas import tpu as pltpu
from jax.sharding import PartitionSpec as P

MESH = pl.DeviceIdType.MESH
LANES = 128
F32, BF16 = jnp.float32, jnp.bfloat16


def rows_dot(left, right):
    return lax.dot_general(left, right, (((0,), (0,)), ((), ())), preferred_element_type=F32)


def cols_dot(left, right):
    return lax.dot_general(left, right, (((1,), (1,)), ((), ())), preferred_element_type=F32)


def plan(n_rep, width, hidden):
    panels = hidden // LANES
    subs = 2 if width * panels // (4 * n_rep) >= 2 * LANES else 1
    per_panel = 2 * n_rep * subs // panels
    return subs, per_panel, width // per_panel


def kernel(
    n_rep, x_ref, pre_ref, cot_ref, wu_hbm, wd_hbm,
    gi_ref, up_ref, down_ref,
    wu, wd, xg, cg, pre_in, sq, gp, pa_own, pa_out, pa_in, gi_out, gi_in,
    first_d, first_u, rs_d, rs_u,
    w_sem, tp_s, tp_r, pre_s, pre_r, gp_s, gp_r, pa_s, pa_r, gi_s, gi_r,
    rsd_s, rsd_r, rsu_s, rsu_r, agd_s, agd_r, agu_s, agu_r,
):
    half, width = x_ref.shape
    hidden = pre_ref.shape[1]
    panels = hidden // LANES
    subs, per_panel, w = plan(n_rep, width, hidden)
    fine = 2 * n_rep == panels
    rep, fs, tp = lax.axis_index("rep"), lax.axis_index("fs"), lax.axis_index("tp")
    line = n_rep // 2
    row, col = rep // 2, rep % 2
    pos = jnp.where(col == 0, row, n_rep - 1 - row)

    def rep_at(p):
        p = lax.rem(p + n_rep, n_rep)
        return jnp.where(p < line, 2 * p, 2 * (n_rep - 1 - p) + 1)

    nxt, prv = rep_at(pos + 1), rep_at(pos + n_rep - 1)
    goal = ({"rep": nxt}, {"rep": prv})
    other_fs, other_tp = {"fs": 1 - fs}, {"tp": 1 - tp}
    mine_f = pl.ds(pl.multiple_of(fs * half, half), half)
    his_f = pl.ds(pl.multiple_of((1 - fs) * half, half), half)
    mine_t = pl.ds(pl.multiple_of(tp * half, half), half)
    his_t = pl.ds(pl.multiple_of((1 - tp) * half, half), half)

    def remote(src, dst, s, r, dev):
        return pltpu.make_async_remote_copy(
            src_ref=src, dst_ref=dst, send_sem=s, recv_sem=r, device_id=dev,
            device_id_type=MESH)

    load_wd = pltpu.make_async_copy(wd_hbm, wd, w_sem.at[0])
    load_wu = pltpu.make_async_copy(wu_hbm, wu, w_sem.at[1])
    load_wd.start()
    load_wu.start()

    barrier = pltpu.get_barrier_semaphore()
    for dev in (goal[0], goal[1], other_fs, other_tp):
        pl.semaphore_signal(barrier, inc=1, device_id=dev, device_id_type=MESH)
    pl.semaphore_wait(barrier, 4)

    def chunk_of(d, j):
        return lax.rem(pos + (-1 - j if d == 0 else 1 + j) + 2 * n_rep, n_rep)

    def lanes(panel):
        return pl.ds(pl.multiple_of(panel * LANES, LANES), LANES)

    def panel_of(d, j):
        return d * n_rep + chunk_of(d, j)

    def pre_copy(panel):
        return remote(pre_ref.at[:, lanes(panel)], pre_in.at[:, lanes(panel)],
                      pre_s.at[panel], pre_r.at[panel], other_fs)

    def gp_copy(panel):
        return remote(gp.at[mine_f, lanes(panel)], gp.at[mine_f, lanes(panel)],
                      gp_s.at[panel], gp_r.at[panel], other_fs)

    def in_order(body):
        if fine:
            def step(j, _):
                body(panel_of(0, j))
                body(panel_of(1, j))
                return 0
            lax.fori_loop(0, n_rep, step, 0)
        else:
            def step(j, _):
                body(j)
                return 0
            lax.fori_loop(0, panels, step, 0)

    cot_move = remote(cot_ref, cg.at[mine_t, :], tp_s.at[0], tp_r.at[0], other_tp)
    x_move = remote(x_ref, xg.at[mine_t, :], tp_s.at[1], tp_r.at[1], other_tp)
    cot_move.start()
    in_order(lambda panel: pre_copy(panel).start())
    x_move.start()
    cg[mine_t, :] = cot_ref[...]
    xg[mine_t, :] = x_ref[...]

    def square_of(block):
        positive = jnp.maximum(block.astype(F32), 0.0)
        return (positive * positive).astype(BF16)

    def own_square(j, _):
        sq[mine_f, lanes(j)] = square_of(pre_ref[:, lanes(j)])
        return 0
    lax.fori_loop(0, panels, own_square, 0)

    def pre_arrived(panel):
        pre_copy(panel).wait_recv()
        sq[his_f, lanes(panel)] = square_of(pre_in[:, lanes(panel)])

    def gp_arrived(panel):
        gp_copy(panel).wait_recv()

    def prepare(body, j):
        if fine:
            body(panel_of(0, j))
            body(panel_of(1, j))

    def where(d, chunk, sub):
        block = (d * n_rep + chunk) * subs + sub
        return lanes(block // per_panel), pl.ds(
            pl.multiple_of(lax.rem(block, per_panel) * w, w), w)

    def down_at(d, chunk, sub):
        hid, wid = where(d, chunk, sub)
        return down_ref.at[hid, wid]

    def up_at(d, chunk, sub):
        hid, wid = where(d, chunk, sub)
        return up_ref.at[wid, hid]

    def down_block(d, chunk, sub):
        hid, wid = where(d, chunk, sub)
        return rows_dot(sq[:, hid], cg[:, wid])

    def up_block(d, chunk, sub):
        hid, wid = where(d, chunk, sub)
        return rows_dot(xg[:, wid], gp[:, hid])

    def rs_copy(first, slots, s_sem, r_sem, d, sub, s, src=None):
        src = slots.at[d, sub, s - 1] if src is None else src
        return remote(src, slots.at[d, sub, s], s_sem.at[d, sub, s], r_sem.at[d, sub, s],
                      goal[d])

    def ag_copy(at, s_sem, r_sem, d, sub, s):
        chunk = lax.rem(pos + (-s if d == 0 else s) + n_rep, n_rep)
        return remote(at(d, chunk, sub), at(d, chunk, sub), s_sem.at[d, sub, s],
                      r_sem.at[d, sub, s], goal[d])

    streams = [(d, sub) for sub in range(subs) for d in range(2)]

    def rs_open(block, first, slots, s_sem, r_sem):
        for d, sub in streams:
            first[d, sub] = block(d, chunk_of(d, 0), sub).astype(BF16)
            rs_copy(first, slots, s_sem, r_sem, d, sub, 0, first.at[d, sub]).start()

    def rs_step(block, first, slots, s_sem, r_sem, j, d, sub):
        part = block(d, chunk_of(d, j), sub)
        rs_copy(first, slots, s_sem, r_sem, d, sub, j - 1, first.at[d, sub]).wait_recv()
        slots[d, sub, j - 1] = (slots[d, sub, j - 1].astype(F32) + part).astype(BF16)
        rs_copy(first, slots, s_sem, r_sem, d, sub, j).start()

    def rs_close(block, at, first, slots, s_sem, r_sem, as_, ar, d, sub):
        part = block(d, pos, sub)
        last = n_rep - 2
        rs_copy(first, slots, s_sem, r_sem, d, sub, last, first.at[d, sub]).wait_recv()
        at(d, pos, sub)[...] = (slots[d, sub, last].astype(F32) + part).astype(BF16)
        ag_copy(at, as_, ar, d, sub, 0).start()

    def ag_step(at, as_, ar, s, d, sub):
        chunk = lax.rem(pos + (-s if d == 0 else s) + n_rep, n_rep)
        remote(at(d, chunk, sub), at(d, chunk, sub), as_.at[d, sub, s - 1],
               ar.at[d, sub, s - 1], goal[d]).wait_recv()
        ag_copy(at, as_, ar, d, sub, s).start()

    def ag_close(at, as_, ar, d, sub):
        s = n_rep - 1
        chunk = lax.rem(pos + (-s if d == 0 else s) + n_rep, n_rep)
        remote(at(d, chunk, sub), at(d, chunk, sub), as_.at[d, sub, s - 1],
               ar.at[d, sub, s - 1], goal[d]).wait_recv()

    down = (first_d, rs_d, rsd_s, rsd_r)
    up = (first_u, rs_u, rsu_s, rsu_r)

    cot_move.wait_recv()
    if fine:
        prepare(pre_arrived, 0)
    else:
        in_order(pre_arrived)
    rs_open(down_block, *down)

    load_wd.wait()
    piece = min(2 * LANES, hidden)

    def act_step(n, _):
        at = pl.ds(pl.multiple_of(n * piece, piece), piece)
        pa_out[:, at] = cols_dot(cg[his_f, :], wd[at, :]).astype(BF16)
        return 0
    lax.fori_loop(0, hidden // piece, act_step, 0)
    pa_move = remote(pa_out, pa_in, pa_s, pa_r, other_fs)
    pa_move.start()

    def act_own(n, _):
        at = pl.ds(pl.multiple_of(n * piece, piece), piece)
        pa_own[:, at] = cols_dot(cg[mine_f, :], wd[at, :])
        return 0
    lax.fori_loop(0, hidden // piece, act_own, 0)

    def down_step(j, _):
        prepare(pre_arrived, j)
        for d, sub in streams:
            rs_step(down_block, *down, j, d, sub)
        return 0
    lax.fori_loop(1, n_rep - 1, down_step, 0)
    prepare(pre_arrived, n_rep - 1)
    for d, sub in streams:
        rs_close(down_block, down_at, *down, agd_s, agd_r, d, sub)

    pa_move.wait_recv()

    def pre_grad(panel):
        at = lanes(panel)
        positive = jnp.maximum(pre_ref[:, at].astype(F32), 0.0)
        grad = pa_own[:, at] + pa_in[:, at].astype(F32)
        gp[mine_f, at] = (2.0 * positive * grad).astype(BF16)
        gp_copy(panel).start()
    in_order(pre_grad)
    x_move.wait_recv()
    if fine:
        prepare(gp_arrived, 0)
    else:
        in_order(gp_arrived)
    rs_open(up_block, *up)

    def both_step(j, _):
        prepare(gp_arrived, j)
        for d, sub in streams:
            ag_step(down_at, agd_s, agd_r, j, d, sub)
            rs_step(up_block, *up, j, d, sub)
        return 0
    lax.fori_loop(1, n_rep - 1, both_step, 0)
    prepare(gp_arrived, n_rep - 1)
    for d, sub in streams:
        ag_close(down_at, agd_s, agd_r, d, sub)
        rs_close(up_block, up_at, *up, agu_s, agu_r, d, sub)

    load_wu.wait()
    wide = min(2 * LANES, width)

    def input_out(n, _):
        at = pl.ds(pl.multiple_of(n * wide, wide), wide)
        gi_out[:, at] = cols_dot(gp[his_t, :], wu[at, :]).astype(BF16)
        return 0
    lax.fori_loop(0, width // wide, input_out, 0)
    gi_move = remote(gi_out, gi_in, gi_s, gi_r, other_tp)
    gi_move.start()

    def gather_step(j, _):
        for d, sub in streams:
            ag_step(up_at, agu_s, agu_r, j, d, sub)
        return 0
    lax.fori_loop(1, n_rep - 1, gather_step, 0)

    gi_move.wait_recv()

    def input_own(n, _):
        at = pl.ds(pl.multiple_of(n * wide, wide), wide)
        own = cols_dot(gp[mine_t, :], wu[at, :]).astype(BF16).astype(F32)
        gi_ref[:, at] = (own + gi_in[:, at].astype(F32)).astype(BF16)
        return 0
    lax.fori_loop(0, width // wide, input_own, 0)
    for d, sub in streams:
        ag_close(up_at, agu_s, agu_r, d, sub)

    for move in (cot_move, x_move, pa_move, gi_move):
        move.wait_send()

    def sent_panels(j, _):
        pre_copy(j).wait_send()
        gp_copy(j).wait_send()
        return 0
    lax.fori_loop(0, panels, sent_panels, 0)

    def sent_steps(s, _):
        for d, sub in streams:
            rs_copy(*down, d, sub, s, first_d.at[d, sub]).wait_send()
            rs_copy(*up, d, sub, s, first_u.at[d, sub]).wait_send()
            ag_copy(down_at, agd_s, agd_r, d, sub, s).wait_send()
            ag_copy(up_at, agu_s, agu_r, d, sub, s).wait_send()
        return 0
    lax.fori_loop(0, n_rep - 1, sent_steps, 0)


def per_device(n_rep, inputs, pre_act, cotangent, up_weight, down_weight):
    half, width = inputs.shape
    hidden = pre_act.shape[1]
    panels = hidden // LANES
    subs, per_panel, w = plan(n_rep, width, hidden)
    dma = pltpu.SemaphoreType.DMA
    ring = [dma((2, subs, n_rep - 1))] * 2
    vmem = pl.BlockSpec(memory_space=pltpu.VMEM)
    anywhere = pl.BlockSpec(memory_space=pl.ANY)
    grad_inputs, grad_up, grad_down = pl.pallas_call(
        functools.partial(kernel, n_rep),
        name="ffn_backward",
        out_shape=(
            pltpu.VMEM((half, width), BF16),
            pltpu.VMEM((width, hidden), BF16),
            pltpu.VMEM((hidden, width), BF16),
        ),
        in_specs=[vmem, vmem, vmem, anywhere, anywhere],
        out_specs=(vmem, vmem, vmem),
        scratch_shapes=[
            pltpu.VMEM((width, hidden), BF16),
            pltpu.VMEM((hidden, width), BF16),
            pltpu.VMEM((2 * half, width), BF16),
            pltpu.VMEM((2 * half, width), BF16),
            pltpu.VMEM((half, hidden), BF16),
            pltpu.VMEM((2 * half, hidden), BF16),
            pltpu.VMEM((2 * half, hidden), BF16),
            pltpu.VMEM((half, hidden), F32),
            pltpu.VMEM((half, hidden), BF16),
            pltpu.VMEM((half, hidden), BF16),
            pltpu.VMEM((half, width), BF16),
            pltpu.VMEM((half, width), BF16),
            pltpu.VMEM((2, subs, LANES, w), BF16),
            pltpu.VMEM((2, subs, w, LANES), BF16),
            pltpu.VMEM((2, subs, n_rep - 1, LANES, w), BF16),
            pltpu.VMEM((2, subs, n_rep - 1, w, LANES), BF16),
            dma((2,)), dma((2,)), dma((2,)),
            dma((panels,)), dma((panels,)), dma((panels,)), dma((panels,)),
            dma, dma, dma, dma,
            *ring, *ring, *ring, *ring,
        ],
        compiler_params=pltpu.CompilerParams(
            collective_id=0, has_side_effects=True, vmem_limit_bytes=48 * 2**20
        ),
    )(inputs, pre_act, cotangent, up_weight, down_weight)
    factor = (half * n_rep * lax.axis_size("tp")) ** (-0.5)
    return grad_inputs, grad_up.astype(F32) * factor, grad_down.astype(F32) * factor


def solution(mesh):
    assert mesh.shape["fs"] == 2 and mesh.shape["tp"] == 2
    placed = (
        P(("rep", "tp"), "fs"),
        P(("rep", "fs"), "tp"),
        P(("rep", "tp"), "fs"),
        P("fs", "tp"),
        P("tp", "fs"),
    )
    return jax.shard_map(
        functools.partial(per_device, mesh.shape["rep"]),
        mesh=mesh,
        in_specs=placed,
        out_specs=(P(("rep", "tp"), "fs"), P("fs", "tp"), P("tp", "fs")),
        check_vma=False,
    )
```

```python
import functools

import jax
import jax.numpy as jnp
from jax import lax
from jax.experimental import pallas as pl
from jax.experimental.pallas import tpu as pltpu
from jax.sharding import PartitionSpec as P

MESH = pl.DeviceIdType.MESH
LANES = 128
F32, BF16 = jnp.float32, jnp.bfloat16


def rows_dot(left, right):
    return lax.dot_general(left, right, (((0,), (0,)), ((), ())), preferred_element_type=F32)


def cols_dot(left, right):
    return lax.dot_general(left, right, (((1,), (1,)), ((), ())), preferred_element_type=F32)


def plan(n_rep, width, hidden):
    panels = hidden // LANES
    room = width * panels // (2 * n_rep)
    subs = max(n for n in (1, 2, 4) if n == 1 or room // n >= 2 * LANES)
    per_panel = 2 * n_rep * subs // panels
    return subs, per_panel, width // per_panel


def kernel(
    n_rep, x_ref, pre_ref, cot_ref, wu_hbm, wd_hbm,
    gi_ref, up_ref, down_ref,
    wu, wd, xg, cg, pre_in, sq, gp, pa_own, pa_out, pa_in, gi_out, gi_in,
    first_d, first_u, rs_d, rs_u,
    w_sem, tp_s, tp_r, pre_s, pre_r, gp_s, gp_r, pa_s, pa_r, gi_s, gi_r,
    rsd_s, rsd_r, rsu_s, rsu_r, agd_s, agd_r, agu_s, agu_r,
):
    half, width = x_ref.shape
    hidden = pre_ref.shape[1]
    panels = hidden // LANES
    subs, per_panel, w = plan(n_rep, width, hidden)
    fine = 2 * n_rep == panels
    rep, fs, tp = lax.axis_index("rep"), lax.axis_index("fs"), lax.axis_index("tp")
    line = n_rep // 2
    row, col = rep // 2, rep % 2
    pos = jnp.where(col == 0, row, n_rep - 1 - row)

    def rep_at(p):
        p = lax.rem(p + n_rep, n_rep)
        return jnp.where(p < line, 2 * p, 2 * (n_rep - 1 - p) + 1)

    nxt, prv = rep_at(pos + 1), rep_at(pos + n_rep - 1)
    goal = ({"rep": nxt}, {"rep": prv})
    other_fs, other_tp = {"fs": 1 - fs}, {"tp": 1 - tp}
    mine_f = pl.ds(pl.multiple_of(fs * half, half), half)
    his_f = pl.ds(pl.multiple_of((1 - fs) * half, half), half)
    mine_t = pl.ds(pl.multiple_of(tp * half, half), half)
    his_t = pl.ds(pl.multiple_of((1 - tp) * half, half), half)

    def remote(src, dst, s, r, dev):
        return pltpu.make_async_remote_copy(
            src_ref=src, dst_ref=dst, send_sem=s, recv_sem=r, device_id=dev,
            device_id_type=MESH)

    load_wd = pltpu.make_async_copy(wd_hbm, wd, w_sem.at[0])
    load_wu = pltpu.make_async_copy(wu_hbm, wu, w_sem.at[1])
    load_wd.start()
    load_wu.start()

    barrier = pltpu.get_barrier_semaphore()
    for dev in (goal[0], goal[1], other_fs, other_tp):
        pl.semaphore_signal(barrier, inc=1, device_id=dev, device_id_type=MESH)
    pl.semaphore_wait(barrier, 4)

    def chunk_of(d, j):
        return lax.rem(pos + (-1 - j if d == 0 else 1 + j) + 2 * n_rep, n_rep)

    def lanes(panel):
        return pl.ds(pl.multiple_of(panel * LANES, LANES), LANES)

    def panel_of(d, j):
        return d * n_rep + chunk_of(d, j)

    def pre_copy(panel):
        return remote(pre_ref.at[:, lanes(panel)], pre_in.at[:, lanes(panel)],
                      pre_s.at[panel], pre_r.at[panel], other_fs)

    def gp_copy(panel):
        return remote(gp.at[mine_f, lanes(panel)], gp.at[mine_f, lanes(panel)],
                      gp_s.at[panel], gp_r.at[panel], other_fs)

    def in_order(body):
        if fine:
            def step(j, _):
                body(panel_of(0, j))
                body(panel_of(1, j))
                return 0
            lax.fori_loop(0, n_rep, step, 0)
        else:
            def step(j, _):
                body(j)
                return 0
            lax.fori_loop(0, panels, step, 0)

    cot_move = remote(cot_ref, cg.at[mine_t, :], tp_s.at[0], tp_r.at[0], other_tp)
    x_move = remote(x_ref, xg.at[mine_t, :], tp_s.at[1], tp_r.at[1], other_tp)
    cot_move.start()
    in_order(lambda panel: pre_copy(panel).start())
    x_move.start()
    cg[mine_t, :] = cot_ref[...]
    xg[mine_t, :] = x_ref[...]

    def square_of(block):
        positive = jnp.maximum(block.astype(F32), 0.0)
        return (positive * positive).astype(BF16)

    def own_square(j, _):
        sq[mine_f, lanes(j)] = square_of(pre_ref[:, lanes(j)])
        return 0
    lax.fori_loop(0, panels, own_square, 0)

    def pre_arrived(panel):
        pre_copy(panel).wait_recv()
        sq[his_f, lanes(panel)] = square_of(pre_in[:, lanes(panel)])

    def gp_arrived(panel):
        gp_copy(panel).wait_recv()

    def prepare(body, j):
        if fine:
            body(panel_of(0, j))
            body(panel_of(1, j))

    def where(d, chunk, sub):
        block = (d * n_rep + chunk) * subs + sub
        return lanes(block // per_panel), pl.ds(
            pl.multiple_of(lax.rem(block, per_panel) * w, w), w)

    def down_at(d, chunk, sub):
        hid, wid = where(d, chunk, sub)
        return down_ref.at[hid, wid]

    def up_at(d, chunk, sub):
        hid, wid = where(d, chunk, sub)
        return up_ref.at[wid, hid]

    def down_block(d, chunk, sub):
        hid, wid = where(d, chunk, sub)
        return rows_dot(sq[:, hid], cg[:, wid])

    def up_block(d, chunk, sub):
        hid, wid = where(d, chunk, sub)
        return rows_dot(xg[:, wid], gp[:, hid])

    def rs_copy(first, slots, s_sem, r_sem, d, sub, s, src=None):
        src = slots.at[d, sub, s - 1] if src is None else src
        return remote(src, slots.at[d, sub, s], s_sem.at[d, sub, s], r_sem.at[d, sub, s],
                      goal[d])

    def ag_copy(at, s_sem, r_sem, d, sub, s):
        chunk = lax.rem(pos + (-s if d == 0 else s) + n_rep, n_rep)
        return remote(at(d, chunk, sub), at(d, chunk, sub), s_sem.at[d, sub, s],
                      r_sem.at[d, sub, s], goal[d])

    streams = [(d, sub) for sub in range(subs) for d in range(2)]

    def rs_open(block, first, slots, s_sem, r_sem):
        for d, sub in streams:
            first[d, sub] = block(d, chunk_of(d, 0), sub).astype(BF16)
            rs_copy(first, slots, s_sem, r_sem, d, sub, 0, first.at[d, sub]).start()

    def rs_step(block, first, slots, s_sem, r_sem, j, d, sub):
        part = block(d, chunk_of(d, j), sub)
        rs_copy(first, slots, s_sem, r_sem, d, sub, j - 1, first.at[d, sub]).wait_recv()
        slots[d, sub, j - 1] = (slots[d, sub, j - 1].astype(F32) + part).astype(BF16)
        rs_copy(first, slots, s_sem, r_sem, d, sub, j).start()

    def rs_close(block, at, first, slots, s_sem, r_sem, as_, ar, d, sub):
        part = block(d, pos, sub)
        last = n_rep - 2
        rs_copy(first, slots, s_sem, r_sem, d, sub, last, first.at[d, sub]).wait_recv()
        at(d, pos, sub)[...] = (slots[d, sub, last].astype(F32) + part).astype(BF16)
        ag_copy(at, as_, ar, d, sub, 0).start()

    def ag_step(at, as_, ar, s, d, sub):
        chunk = lax.rem(pos + (-s if d == 0 else s) + n_rep, n_rep)
        remote(at(d, chunk, sub), at(d, chunk, sub), as_.at[d, sub, s - 1],
               ar.at[d, sub, s - 1], goal[d]).wait_recv()
        ag_copy(at, as_, ar, d, sub, s).start()

    def ag_close(at, as_, ar, d, sub):
        s = n_rep - 1
        chunk = lax.rem(pos + (-s if d == 0 else s) + n_rep, n_rep)
        remote(at(d, chunk, sub), at(d, chunk, sub), as_.at[d, sub, s - 1],
               ar.at[d, sub, s - 1], goal[d]).wait_recv()

    down = (first_d, rs_d, rsd_s, rsd_r)
    up = (first_u, rs_u, rsu_s, rsu_r)

    cot_move.wait_recv()
    if fine:
        prepare(pre_arrived, 0)
    else:
        in_order(pre_arrived)
    rs_open(down_block, *down)

    load_wd.wait()
    piece = min(2 * LANES, hidden)

    def act_step(n, _):
        at = pl.ds(pl.multiple_of(n * piece, piece), piece)
        pa_out[:, at] = cols_dot(cg[his_f, :], wd[at, :]).astype(BF16)
        return 0
    lax.fori_loop(0, hidden // piece, act_step, 0)
    pa_move = remote(pa_out, pa_in, pa_s, pa_r, other_fs)
    pa_move.start()

    def act_own(n, _):
        at = pl.ds(pl.multiple_of(n * piece, piece), piece)
        pa_own[:, at] = cols_dot(cg[mine_f, :], wd[at, :])
        return 0
    lax.fori_loop(0, hidden // piece, act_own, 0)

    def down_step(j, _):
        prepare(pre_arrived, j)
        for d, sub in streams:
            rs_step(down_block, *down, j, d, sub)
        return 0
    lax.fori_loop(1, n_rep - 1, down_step, 0)
    prepare(pre_arrived, n_rep - 1)
    for d, sub in streams:
        rs_close(down_block, down_at, *down, agd_s, agd_r, d, sub)

    pa_move.wait_recv()

    def pre_grad(panel):
        at = lanes(panel)
        positive = jnp.maximum(pre_ref[:, at].astype(F32), 0.0)
        grad = pa_own[:, at] + pa_in[:, at].astype(F32)
        gp[mine_f, at] = (2.0 * positive * grad).astype(BF16)
        gp_copy(panel).start()
    in_order(pre_grad)
    x_move.wait_recv()
    for d, sub in streams:
        ag_step(down_at, agd_s, agd_r, 1, d, sub)
    if fine:
        prepare(gp_arrived, 0)
    else:
        in_order(gp_arrived)
    rs_open(up_block, *up)

    def both_step(j, _):
        prepare(gp_arrived, j)
        for d, sub in streams:
            ag_step(down_at, agd_s, agd_r, j + 1, d, sub)
            rs_step(up_block, *up, j, d, sub)
        return 0
    lax.fori_loop(1, n_rep - 2, both_step, 0)
    prepare(gp_arrived, n_rep - 2)
    for d, sub in streams:
        rs_step(up_block, *up, n_rep - 2, d, sub)
    prepare(gp_arrived, n_rep - 1)
    for d, sub in streams:
        ag_close(down_at, agd_s, agd_r, d, sub)
        rs_close(up_block, up_at, *up, agu_s, agu_r, d, sub)

    load_wu.wait()
    wide = min(2 * LANES, width)

    def input_out(n, _):
        at = pl.ds(pl.multiple_of(n * wide, wide), wide)
        gi_out[:, at] = cols_dot(gp[his_t, :], wu[at, :]).astype(BF16)
        return 0
    lax.fori_loop(0, width // wide, input_out, 0)
    gi_move = remote(gi_out, gi_in, gi_s, gi_r, other_tp)
    gi_move.start()

    def gather_step(j, _):
        for d, sub in streams:
            ag_step(up_at, agu_s, agu_r, j, d, sub)
        return 0
    lax.fori_loop(1, n_rep - 1, gather_step, 0)

    gi_move.wait_recv()

    def input_own(n, _):
        at = pl.ds(pl.multiple_of(n * wide, wide), wide)
        own = cols_dot(gp[mine_t, :], wu[at, :]).astype(BF16).astype(F32)
        gi_ref[:, at] = (own + gi_in[:, at].astype(F32)).astype(BF16)
        return 0
    lax.fori_loop(0, width // wide, input_own, 0)
    for d, sub in streams:
        ag_close(up_at, agu_s, agu_r, d, sub)

    for move in (cot_move, x_move, pa_move, gi_move):
        move.wait_send()

    def sent_panels(j, _):
        pre_copy(j).wait_send()
        gp_copy(j).wait_send()
        return 0
    lax.fori_loop(0, panels, sent_panels, 0)

    def sent_steps(s, _):
        for d, sub in streams:
            rs_copy(*down, d, sub, s, first_d.at[d, sub]).wait_send()
            rs_copy(*up, d, sub, s, first_u.at[d, sub]).wait_send()
            ag_copy(down_at, agd_s, agd_r, d, sub, s).wait_send()
            ag_copy(up_at, agu_s, agu_r, d, sub, s).wait_send()
        return 0
    lax.fori_loop(0, n_rep - 1, sent_steps, 0)


def per_device(n_rep, inputs, pre_act, cotangent, up_weight, down_weight):
    half, width = inputs.shape
    hidden = pre_act.shape[1]
    panels = hidden // LANES
    subs, per_panel, w = plan(n_rep, width, hidden)
    dma = pltpu.SemaphoreType.DMA
    ring = [dma((2, subs, n_rep - 1))] * 2
    vmem = pl.BlockSpec(memory_space=pltpu.VMEM)
    anywhere = pl.BlockSpec(memory_space=pl.ANY)
    grad_inputs, grad_up, grad_down = pl.pallas_call(
        functools.partial(kernel, n_rep),
        name="ffn_backward",
        out_shape=(
            pltpu.VMEM((half, width), BF16),
            pltpu.VMEM((width, hidden), BF16),
            pltpu.VMEM((hidden, width), BF16),
        ),
        in_specs=[vmem, vmem, vmem, anywhere, anywhere],
        out_specs=(vmem, vmem, vmem),
        scratch_shapes=[
            pltpu.VMEM((width, hidden), BF16),
            pltpu.VMEM((hidden, width), BF16),
            pltpu.VMEM((2 * half, width), BF16),
            pltpu.VMEM((2 * half, width), BF16),
            pltpu.VMEM((half, hidden), BF16),
            pltpu.VMEM((2 * half, hidden), BF16),
            pltpu.VMEM((2 * half, hidden), BF16),
            pltpu.VMEM((half, hidden), F32),
            pltpu.VMEM((half, hidden), BF16),
            pltpu.VMEM((half, hidden), BF16),
            pltpu.VMEM((half, width), BF16),
            pltpu.VMEM((half, width), BF16),
            pltpu.VMEM((2, subs, LANES, w), BF16),
            pltpu.VMEM((2, subs, w, LANES), BF16),
            pltpu.VMEM((2, subs, n_rep - 1, LANES, w), BF16),
            pltpu.VMEM((2, subs, n_rep - 1, w, LANES), BF16),
            dma((2,)), dma((2,)), dma((2,)),
            dma((panels,)), dma((panels,)), dma((panels,)), dma((panels,)),
            dma, dma, dma, dma,
            *ring, *ring, *ring, *ring,
        ],
        compiler_params=pltpu.CompilerParams(
            collective_id=0, has_side_effects=True, vmem_limit_bytes=50 * 2**20
        ),
    )(inputs, pre_act, cotangent, up_weight, down_weight)
    factor = (half * n_rep * lax.axis_size("tp")) ** (-0.5)
    return grad_inputs, grad_up.astype(F32) * factor, grad_down.astype(F32) * factor


def solution(mesh):
    assert mesh.shape["fs"] == 2 and mesh.shape["tp"] == 2
    placed = (
        P(("rep", "tp"), "fs"),
        P(("rep", "fs"), "tp"),
        P(("rep", "tp"), "fs"),
        P("fs", "tp"),
        P("tp", "fs"),
    )
    return jax.shard_map(
        functools.partial(per_device, mesh.shape["rep"]),
        mesh=mesh,
        in_specs=placed,
        out_specs=(P(("rep", "tp"), "fs"), P("fs", "tp"), P("tp", "fs")),
        check_vma=False,
    )
```

```python
import functools

import jax
import jax.numpy as jnp
from jax import lax
from jax.experimental import pallas as pl
from jax.experimental.pallas import tpu as pltpu
from jax.sharding import PartitionSpec as P

MESH = pl.DeviceIdType.MESH
LANES = 128
F32, BF16 = jnp.float32, jnp.bfloat16


def rows_dot(left, right):
    return lax.dot_general(left, right, (((0,), (0,)), ((), ())), preferred_element_type=F32)


def cols_dot(left, right):
    return lax.dot_general(left, right, (((1,), (1,)), ((), ())), preferred_element_type=F32)


def plan(n_rep, width, hidden):
    panels = hidden // LANES
    room = width * panels // (2 * n_rep)
    subs = max(n for n in (1, 2, 4) if n == 1 or room // n >= 2 * LANES)
    per_panel = 2 * n_rep * subs // panels
    return subs, per_panel, width // per_panel


def kernel(
    n_rep, x_hbm, pre_hbm, cot_hbm, wu_hbm, wd_hbm,
    gi_ref, up_ref, down_ref,
    x_ref, pre_ref, cot_ref, wu, wd, xg, cg, pre_in, sq, gp, pa_own, pa_out, pa_in, gi_out, gi_in,
    first_d, first_u, rs_d, rs_u,
    w_sem, tp_s, tp_r, pre_s, pre_r, gp_s, gp_r, pa_s, pa_r, gi_s, gi_r,
    rsd_s, rsd_r, rsu_s, rsu_r, agd_s, agd_r, agu_s, agu_r,
):
    half, width = x_ref.shape
    hidden = pre_ref.shape[1]
    panels = hidden // LANES
    subs, per_panel, w = plan(n_rep, width, hidden)
    fine = 2 * n_rep == panels
    rep, fs, tp = lax.axis_index("rep"), lax.axis_index("fs"), lax.axis_index("tp")
    line = n_rep // 2
    row, col = rep // 2, rep % 2
    pos = jnp.where(col == 0, row, n_rep - 1 - row)

    def rep_at(p):
        p = lax.rem(p + n_rep, n_rep)
        return jnp.where(p < line, 2 * p, 2 * (n_rep - 1 - p) + 1)

    nxt, prv = rep_at(pos + 1), rep_at(pos + n_rep - 1)
    goal = ({"rep": nxt}, {"rep": prv})
    other_fs, other_tp = {"fs": 1 - fs}, {"tp": 1 - tp}
    mine_f = pl.ds(pl.multiple_of(fs * half, half), half)
    his_f = pl.ds(pl.multiple_of((1 - fs) * half, half), half)
    mine_t = pl.ds(pl.multiple_of(tp * half, half), half)
    his_t = pl.ds(pl.multiple_of((1 - tp) * half, half), half)

    def remote(src, dst, s, r, dev):
        return pltpu.make_async_remote_copy(
            src_ref=src, dst_ref=dst, send_sem=s, recv_sem=r, device_id=dev,
            device_id_type=MESH)

    barrier = pltpu.get_barrier_semaphore()
    for dev in (goal[0], goal[1], other_fs, other_tp):
        pl.semaphore_signal(barrier, inc=1, device_id=dev, device_id_type=MESH)
    held = ((cot_hbm, cot_ref), (pre_hbm, pre_ref), (x_hbm, x_ref), (wd_hbm, wd), (wu_hbm, wu))
    loads = [pltpu.make_async_copy(src, dst, w_sem.at[i]) for i, (src, dst) in enumerate(held)]
    load_cot, load_pre, load_x, load_wd, load_wu = loads
    for load in loads:
        load.start()
    load_cot.wait()
    load_pre.wait()
    pl.semaphore_wait(barrier, 4)

    def chunk_of(d, j):
        return lax.rem(pos + (-1 - j if d == 0 else 1 + j) + 2 * n_rep, n_rep)

    def lanes(panel):
        return pl.ds(pl.multiple_of(panel * LANES, LANES), LANES)

    def panel_of(d, j):
        return d * n_rep + chunk_of(d, j)

    def pre_copy(panel):
        return remote(pre_ref.at[:, lanes(panel)], pre_in.at[:, lanes(panel)],
                      pre_s.at[panel], pre_r.at[panel], other_fs)

    def gp_copy(panel):
        return remote(gp.at[mine_f, lanes(panel)], gp.at[mine_f, lanes(panel)],
                      gp_s.at[panel], gp_r.at[panel], other_fs)

    def in_order(body):
        if fine:
            def step(j, _):
                body(panel_of(0, j))
                body(panel_of(1, j))
                return 0
            lax.fori_loop(0, n_rep, step, 0)
        else:
            def step(j, _):
                body(j)
                return 0
            lax.fori_loop(0, panels, step, 0)

    cot_move = remote(cot_ref, cg.at[mine_t, :], tp_s.at[0], tp_r.at[0], other_tp)
    x_move = remote(x_ref, xg.at[mine_t, :], tp_s.at[1], tp_r.at[1], other_tp)
    cot_move.start()
    in_order(lambda panel: pre_copy(panel).start())
    load_x.wait()
    x_move.start()
    cg[mine_t, :] = cot_ref[...]
    xg[mine_t, :] = x_ref[...]

    def square_of(block):
        positive = jnp.maximum(block.astype(F32), 0.0)
        return (positive * positive).astype(BF16)

    def own_square(j, _):
        sq[mine_f, lanes(j)] = square_of(pre_ref[:, lanes(j)])
        return 0
    lax.fori_loop(0, panels, own_square, 0)

    def pre_arrived(panel):
        pre_copy(panel).wait_recv()
        sq[his_f, lanes(panel)] = square_of(pre_in[:, lanes(panel)])

    def gp_arrived(panel):
        gp_copy(panel).wait_recv()

    def prepare(body, j):
        if fine:
            body(panel_of(0, j))
            body(panel_of(1, j))

    def where(d, chunk, sub):
        block = (d * n_rep + chunk) * subs + sub
        return lanes(block // per_panel), pl.ds(
            pl.multiple_of(lax.rem(block, per_panel) * w, w), w)

    def down_at(d, chunk, sub):
        hid, wid = where(d, chunk, sub)
        return down_ref.at[hid, wid]

    def up_at(d, chunk, sub):
        hid, wid = where(d, chunk, sub)
        return up_ref.at[wid, hid]

    def down_block(d, chunk, sub):
        hid, wid = where(d, chunk, sub)
        return rows_dot(sq[:, hid], cg[:, wid])

    def up_block(d, chunk, sub):
        hid, wid = where(d, chunk, sub)
        return rows_dot(xg[:, wid], gp[:, hid])

    def rs_copy(first, slots, s_sem, r_sem, d, sub, s, src=None):
        src = slots.at[d, sub, s - 1] if src is None else src
        return remote(src, slots.at[d, sub, s], s_sem.at[d, sub, s], r_sem.at[d, sub, s],
                      goal[d])

    def ag_copy(at, s_sem, r_sem, d, sub, s):
        chunk = lax.rem(pos + (-s if d == 0 else s) + n_rep, n_rep)
        return remote(at(d, chunk, sub), at(d, chunk, sub), s_sem.at[d, sub, s],
                      r_sem.at[d, sub, s], goal[d])

    streams = [(d, sub) for sub in range(subs) for d in range(2)]

    def rs_open(block, first, slots, s_sem, r_sem):
        for d, sub in streams:
            first[d, sub] = block(d, chunk_of(d, 0), sub).astype(BF16)
            rs_copy(first, slots, s_sem, r_sem, d, sub, 0, first.at[d, sub]).start()

    def rs_step(block, first, slots, s_sem, r_sem, j, d, sub):
        part = block(d, chunk_of(d, j), sub)
        rs_copy(first, slots, s_sem, r_sem, d, sub, j - 1, first.at[d, sub]).wait_recv()
        slots[d, sub, j - 1] = (slots[d, sub, j - 1].astype(F32) + part).astype(BF16)
        rs_copy(first, slots, s_sem, r_sem, d, sub, j).start()

    def rs_close(block, at, first, slots, s_sem, r_sem, as_, ar, d, sub):
        part = block(d, pos, sub)
        last = n_rep - 2
        rs_copy(first, slots, s_sem, r_sem, d, sub, last, first.at[d, sub]).wait_recv()
        at(d, pos, sub)[...] = (slots[d, sub, last].astype(F32) + part).astype(BF16)
        ag_copy(at, as_, ar, d, sub, 0).start()

    def ag_step(at, as_, ar, s, d, sub):
        chunk = lax.rem(pos + (-s if d == 0 else s) + n_rep, n_rep)
        remote(at(d, chunk, sub), at(d, chunk, sub), as_.at[d, sub, s - 1],
               ar.at[d, sub, s - 1], goal[d]).wait_recv()
        ag_copy(at, as_, ar, d, sub, s).start()

    def ag_close(at, as_, ar, d, sub):
        s = n_rep - 1
        chunk = lax.rem(pos + (-s if d == 0 else s) + n_rep, n_rep)
        remote(at(d, chunk, sub), at(d, chunk, sub), as_.at[d, sub, s - 1],
               ar.at[d, sub, s - 1], goal[d]).wait_recv()

    down = (first_d, rs_d, rsd_s, rsd_r)
    up = (first_u, rs_u, rsu_s, rsu_r)

    cot_move.wait_recv()
    if fine:
        prepare(pre_arrived, 0)
    else:
        in_order(pre_arrived)
    rs_open(down_block, *down)

    load_wd.wait()
    piece = min(2 * LANES, hidden)

    def act_step(n, _):
        at = pl.ds(pl.multiple_of(n * piece, piece), piece)
        pa_out[:, at] = cols_dot(cg[his_f, :], wd[at, :]).astype(BF16)
        return 0
    lax.fori_loop(0, hidden // piece, act_step, 0)
    pa_move = remote(pa_out, pa_in, pa_s, pa_r, other_fs)
    pa_move.start()

    def act_own(n, _):
        at = pl.ds(pl.multiple_of(n * piece, piece), piece)
        pa_own[:, at] = cols_dot(cg[mine_f, :], wd[at, :])
        return 0
    lax.fori_loop(0, hidden // piece, act_own, 0)

    def down_step(j, _):
        prepare(pre_arrived, j)
        for d, sub in streams:
            rs_step(down_block, *down, j, d, sub)
        return 0
    lax.fori_loop(1, n_rep - 1, down_step, 0)
    prepare(pre_arrived, n_rep - 1)
    for d, sub in streams:
        rs_close(down_block, down_at, *down, agd_s, agd_r, d, sub)

    pa_move.wait_recv()

    def pre_grad(panel):
        at = lanes(panel)
        positive = jnp.maximum(pre_ref[:, at].astype(F32), 0.0)
        grad = pa_own[:, at] + pa_in[:, at].astype(F32)
        gp[mine_f, at] = (2.0 * positive * grad).astype(BF16)
        gp_copy(panel).start()
    in_order(pre_grad)
    x_move.wait_recv()
    for d, sub in streams:
        ag_step(down_at, agd_s, agd_r, 1, d, sub)
    if fine:
        prepare(gp_arrived, 0)
    else:
        in_order(gp_arrived)
    rs_open(up_block, *up)

    def both_step(j, _):
        prepare(gp_arrived, j)
        for d, sub in streams:
            ag_step(down_at, agd_s, agd_r, j + 1, d, sub)
            rs_step(up_block, *up, j, d, sub)
        return 0
    lax.fori_loop(1, n_rep - 2, both_step, 0)
    prepare(gp_arrived, n_rep - 2)
    for d, sub in streams:
        rs_step(up_block, *up, n_rep - 2, d, sub)
    prepare(gp_arrived, n_rep - 1)
    for d, sub in streams:
        ag_close(down_at, agd_s, agd_r, d, sub)
        rs_close(up_block, up_at, *up, agu_s, agu_r, d, sub)

    load_wu.wait()
    wide = min(2 * LANES, width)

    def input_out(n, _):
        at = pl.ds(pl.multiple_of(n * wide, wide), wide)
        gi_out[:, at] = cols_dot(gp[his_t, :], wu[at, :]).astype(BF16)
        return 0
    lax.fori_loop(0, width // wide, input_out, 0)
    gi_move = remote(gi_out, gi_in, gi_s, gi_r, other_tp)
    gi_move.start()

    def gather_step(j, _):
        for d, sub in streams:
            ag_step(up_at, agu_s, agu_r, j, d, sub)
        return 0
    lax.fori_loop(1, n_rep - 1, gather_step, 0)

    gi_move.wait_recv()

    def input_own(n, _):
        at = pl.ds(pl.multiple_of(n * wide, wide), wide)
        own = cols_dot(gp[mine_t, :], wu[at, :]).astype(BF16).astype(F32)
        gi_ref[:, at] = (own + gi_in[:, at].astype(F32)).astype(BF16)
        return 0
    lax.fori_loop(0, width // wide, input_own, 0)
    for d, sub in streams:
        ag_close(up_at, agu_s, agu_r, d, sub)

    for move in (cot_move, x_move, pa_move, gi_move):
        move.wait_send()

    def sent_panels(j, _):
        pre_copy(j).wait_send()
        gp_copy(j).wait_send()
        return 0
    lax.fori_loop(0, panels, sent_panels, 0)

    def sent_steps(s, _):
        for d, sub in streams:
            rs_copy(*down, d, sub, s, first_d.at[d, sub]).wait_send()
            rs_copy(*up, d, sub, s, first_u.at[d, sub]).wait_send()
            ag_copy(down_at, agd_s, agd_r, d, sub, s).wait_send()
            ag_copy(up_at, agu_s, agu_r, d, sub, s).wait_send()
        return 0
    lax.fori_loop(0, n_rep - 1, sent_steps, 0)


def scale_kernel(factor, pieces, gi, up, down, gi_out, up_out, down_out, up_wide, down_wide,
                 sems, gi_sem):
    copies = [pltpu.make_async_copy(gi, gi_out, gi_sem)]
    copies[0].start()
    for i in range(pieces):
        for n, (src, wide, dst) in enumerate(((up, up_wide, up_out), (down, down_wide, down_out))):
            rows = pl.ds(i * (src.shape[0] // pieces), src.shape[0] // pieces)
            wide[rows, :] = src[rows, :].astype(F32) * factor
            copy = pltpu.make_async_copy(wide.at[rows, :], dst.at[rows, :], sems.at[n, i])
            copy.start()
            copies.append(copy)
    for copy in copies:
        copy.wait()


def per_device(n_rep, inputs, pre_act, cotangent, up_weight, down_weight):
    half, width = inputs.shape
    hidden = pre_act.shape[1]
    panels = hidden // LANES
    subs, per_panel, w = plan(n_rep, width, hidden)
    dma = pltpu.SemaphoreType.DMA
    ring = [dma((2, subs, n_rep - 1))] * 2
    vmem = pl.BlockSpec(memory_space=pltpu.VMEM)
    anywhere = pl.BlockSpec(memory_space=pl.ANY)
    grad_inputs, grad_up, grad_down = pl.pallas_call(
        functools.partial(kernel, n_rep),
        name="ffn_backward",
        out_shape=(
            pltpu.VMEM((half, width), BF16),
            pltpu.VMEM((width, hidden), BF16),
            pltpu.VMEM((hidden, width), BF16),
        ),
        in_specs=[anywhere] * 5,
        out_specs=(vmem, vmem, vmem),
        scratch_shapes=[
            pltpu.VMEM((half, width), BF16),
            pltpu.VMEM((half, hidden), BF16),
            pltpu.VMEM((half, width), BF16),
            pltpu.VMEM((width, hidden), BF16),
            pltpu.VMEM((hidden, width), BF16),
            pltpu.VMEM((2 * half, width), BF16),
            pltpu.VMEM((2 * half, width), BF16),
            pltpu.VMEM((half, hidden), BF16),
            pltpu.VMEM((2 * half, hidden), BF16),
            pltpu.VMEM((2 * half, hidden), BF16),
            pltpu.VMEM((half, hidden), F32),
            pltpu.VMEM((half, hidden), BF16),
            pltpu.VMEM((half, hidden), BF16),
            pltpu.VMEM((half, width), BF16),
            pltpu.VMEM((half, width), BF16),
            pltpu.VMEM((2, subs, LANES, w), BF16),
            pltpu.VMEM((2, subs, w, LANES), BF16),
            pltpu.VMEM((2, subs, n_rep - 1, LANES, w), BF16),
            pltpu.VMEM((2, subs, n_rep - 1, w, LANES), BF16),
            dma((5,)), dma((2,)), dma((2,)),
            dma((panels,)), dma((panels,)), dma((panels,)), dma((panels,)),
            dma, dma, dma, dma,
            *ring, *ring, *ring, *ring,
        ],
        compiler_params=pltpu.CompilerParams(
            collective_id=0, has_side_effects=True, vmem_limit_bytes=50 * 2**20
        ),
    )(inputs, pre_act, cotangent, up_weight, down_weight)
    factor = (half * n_rep * lax.axis_size("tp")) ** (-0.5)
    pieces = 8
    return pl.pallas_call(
        functools.partial(scale_kernel, factor, pieces),
        name="scale_outputs",
        out_shape=(
            jax.ShapeDtypeStruct((half, width), BF16),
            jax.ShapeDtypeStruct((width, hidden), F32),
            jax.ShapeDtypeStruct((hidden, width), F32),
        ),
        in_specs=[vmem] * 3,
        out_specs=[anywhere] * 3,
        scratch_shapes=[
            pltpu.VMEM((width, hidden), F32),
            pltpu.VMEM((hidden, width), F32),
            dma((2, pieces)),
            dma,
        ],
        compiler_params=pltpu.CompilerParams(vmem_limit_bytes=40 * 2**20),
    )(*[pltpu.with_memory_space_constraint(g, pltpu.VMEM)
        for g in (grad_inputs, grad_up, grad_down)])


def solution(mesh):
    assert mesh.shape["fs"] == 2 and mesh.shape["tp"] == 2
    placed = (
        P(("rep", "tp"), "fs"),
        P(("rep", "fs"), "tp"),
        P(("rep", "tp"), "fs"),
        P("fs", "tp"),
        P("tp", "fs"),
    )
    return jax.shard_map(
        functools.partial(per_device, mesh.shape["rep"]),
        mesh=mesh,
        in_specs=placed,
        out_specs=(P(("rep", "tp"), "fs"), P("fs", "tp"), P("tp", "fs")),
        check_vma=False,
    )
```

```python
import functools

import jax
import jax.numpy as jnp
from jax import lax
from jax.experimental import pallas as pl
from jax.experimental.pallas import tpu as pltpu
from jax.sharding import PartitionSpec as P

MESH = pl.DeviceIdType.MESH
LANES = 128
F32, BF16 = jnp.float32, jnp.bfloat16


def rows_dot(left, right):
    return lax.dot_general(left, right, (((0,), (0,)), ((), ())), preferred_element_type=F32)


def cols_dot(left, right):
    return lax.dot_general(left, right, (((1,), (1,)), ((), ())), preferred_element_type=F32)


def plan(n_rep, width, hidden):
    panels = hidden // LANES
    room = width * panels // (2 * n_rep)
    subs = max(n for n in (1, 2) if n == 1 or room // n >= 2 * LANES)
    per_panel = 2 * n_rep * subs // panels
    return subs, per_panel, width // per_panel


def kernel(
    n_rep, x_hbm, pre_hbm, cot_hbm, wu_hbm, wd_hbm,
    gi_ref, up_ref, down_ref,
    x_ref, pre_ref, cot_ref, wu, wd, xg, cg, pre_in, sq, gp, pa_own, pa_out, pa_in, gi_out, gi_in,
    first_d, first_u, rs_d, rs_u,
    w_sem, tp_s, tp_r, pre_s, pre_r, gp_s, gp_r, pa_s, pa_r, gi_s, gi_r,
    rsd_s, rsd_r, rsu_s, rsu_r, agd_s, agd_r, agu_s, agu_r,
):
    half, width = x_ref.shape
    hidden = pre_ref.shape[1]
    panels = hidden // LANES
    subs, per_panel, w = plan(n_rep, width, hidden)
    fine = 2 * n_rep == panels
    rep, fs, tp = lax.axis_index("rep"), lax.axis_index("fs"), lax.axis_index("tp")
    line = n_rep // 2
    row, col = rep // 2, rep % 2
    pos = jnp.where(col == 0, row, n_rep - 1 - row)

    def rep_at(p):
        p = lax.rem(p + n_rep, n_rep)
        return jnp.where(p < line, 2 * p, 2 * (n_rep - 1 - p) + 1)

    nxt, prv = rep_at(pos + 1), rep_at(pos + n_rep - 1)
    goal = ({"rep": nxt}, {"rep": prv})
    other_fs, other_tp = {"fs": 1 - fs}, {"tp": 1 - tp}
    mine_f = pl.ds(pl.multiple_of(fs * half, half), half)
    his_f = pl.ds(pl.multiple_of((1 - fs) * half, half), half)
    mine_t = pl.ds(pl.multiple_of(tp * half, half), half)
    his_t = pl.ds(pl.multiple_of((1 - tp) * half, half), half)

    def remote(src, dst, s, r, dev):
        return pltpu.make_async_remote_copy(
            src_ref=src, dst_ref=dst, send_sem=s, recv_sem=r, device_id=dev,
            device_id_type=MESH)

    barrier = pltpu.get_barrier_semaphore()
    for dev in (goal[0], goal[1], other_fs, other_tp):
        pl.semaphore_signal(barrier, inc=1, device_id=dev, device_id_type=MESH)
    held = ((cot_hbm, cot_ref), (pre_hbm, pre_ref), (x_hbm, x_ref), (wd_hbm, wd), (wu_hbm, wu))
    loads = [pltpu.make_async_copy(src, dst, w_sem.at[i]) for i, (src, dst) in enumerate(held)]
    load_cot, load_pre, load_x, load_wd, load_wu = loads
    for load in loads:
        load.start()
    load_cot.wait()
    load_pre.wait()
    pl.semaphore_wait(barrier, 4)

    def chunk_of(d, j):
        return lax.rem(pos + (-1 - j if d == 0 else 1 + j) + 2 * n_rep, n_rep)

    def lanes(panel):
        return pl.ds(pl.multiple_of(panel * LANES, LANES), LANES)

    def panel_of(d, j):
        return d * n_rep + chunk_of(d, j)

    def pre_copy(panel):
        return remote(pre_ref.at[:, lanes(panel)], pre_in.at[:, lanes(panel)],
                      pre_s.at[panel], pre_r.at[panel], other_fs)

    def gp_copy(panel):
        return remote(gp.at[mine_f, lanes(panel)], gp.at[mine_f, lanes(panel)],
                      gp_s.at[panel], gp_r.at[panel], other_fs)

    def in_order(body):
        if fine:
            def step(j, _):
                body(panel_of(0, j))
                body(panel_of(1, j))
                return 0
            lax.fori_loop(0, n_rep, step, 0)
        else:
            def step(j, _):
                body(j)
                return 0
            lax.fori_loop(0, panels, step, 0)

    cot_move = remote(cot_ref, cg.at[mine_t, :], tp_s.at[0], tp_r.at[0], other_tp)
    x_move = remote(x_ref, xg.at[mine_t, :], tp_s.at[1], tp_r.at[1], other_tp)
    cot_move.start()
    in_order(lambda panel: pre_copy(panel).start())
    load_x.wait()
    x_move.start()
    cg[mine_t, :] = cot_ref[...]
    xg[mine_t, :] = x_ref[...]

    def square_of(block):
        positive = jnp.maximum(block.astype(F32), 0.0)
        return (positive * positive).astype(BF16)

    def own_square(j, _):
        sq[mine_f, lanes(j)] = square_of(pre_ref[:, lanes(j)])
        return 0
    lax.fori_loop(0, panels, own_square, 0)

    def pre_arrived(panel):
        pre_copy(panel).wait_recv()
        sq[his_f, lanes(panel)] = square_of(pre_in[:, lanes(panel)])

    def gp_arrived(panel):
        gp_copy(panel).wait_recv()

    def prepare(body, j):
        if fine:
            body(panel_of(0, j))
            body(panel_of(1, j))

    def where(d, chunk, sub):
        block = (d * n_rep + chunk) * subs + sub
        return lanes(block // per_panel), pl.ds(
            pl.multiple_of(lax.rem(block, per_panel) * w, w), w)

    def down_at(d, chunk, sub):
        hid, wid = where(d, chunk, sub)
        return down_ref.at[hid, wid]

    def up_at(d, chunk, sub):
        hid, wid = where(d, chunk, sub)
        return up_ref.at[wid, hid]

    def down_block(d, chunk, sub):
        hid, wid = where(d, chunk, sub)
        return rows_dot(sq[:, hid], cg[:, wid])

    def up_block(d, chunk, sub):
        hid, wid = where(d, chunk, sub)
        return rows_dot(xg[:, wid], gp[:, hid])

    def rs_copy(first, slots, s_sem, r_sem, d, sub, s, src=None):
        src = slots.at[d, sub, s - 1] if src is None else src
        return remote(src, slots.at[d, sub, s], s_sem.at[d, sub, s], r_sem.at[d, sub, s],
                      goal[d])

    def ag_copy(at, s_sem, r_sem, d, sub, s):
        chunk = lax.rem(pos + (-s if d == 0 else s) + n_rep, n_rep)
        return remote(at(d, chunk, sub), at(d, chunk, sub), s_sem.at[d, sub, s],
                      r_sem.at[d, sub, s], goal[d])

    streams = [(d, sub) for sub in range(subs) for d in range(2)]

    def rs_open(block, first, slots, s_sem, r_sem):
        for d, sub in streams:
            first[d, sub] = block(d, chunk_of(d, 0), sub).astype(BF16)
            rs_copy(first, slots, s_sem, r_sem, d, sub, 0, first.at[d, sub]).start()

    def rs_step(block, first, slots, s_sem, r_sem, j, d, sub):
        part = block(d, chunk_of(d, j), sub)
        rs_copy(first, slots, s_sem, r_sem, d, sub, j - 1, first.at[d, sub]).wait_recv()
        slots[d, sub, j - 1] = (slots[d, sub, j - 1].astype(F32) + part).astype(BF16)
        rs_copy(first, slots, s_sem, r_sem, d, sub, j).start()

    def rs_close(block, at, first, slots, s_sem, r_sem, as_, ar, d, sub):
        part = block(d, pos, sub)
        last = n_rep - 2
        rs_copy(first, slots, s_sem, r_sem, d, sub, last, first.at[d, sub]).wait_recv()
        at(d, pos, sub)[...] = (slots[d, sub, last].astype(F32) + part).astype(BF16)
        ag_copy(at, as_, ar, d, sub, 0).start()

    def ag_step(at, as_, ar, s, d, sub):
        chunk = lax.rem(pos + (-s if d == 0 else s) + n_rep, n_rep)
        remote(at(d, chunk, sub), at(d, chunk, sub), as_.at[d, sub, s - 1],
               ar.at[d, sub, s - 1], goal[d]).wait_recv()
        ag_copy(at, as_, ar, d, sub, s).start()

    def ag_close(at, as_, ar, d, sub):
        s = n_rep - 1
        chunk = lax.rem(pos + (-s if d == 0 else s) + n_rep, n_rep)
        remote(at(d, chunk, sub), at(d, chunk, sub), as_.at[d, sub, s - 1],
               ar.at[d, sub, s - 1], goal[d]).wait_recv()

    down = (first_d, rs_d, rsd_s, rsd_r)
    up = (first_u, rs_u, rsu_s, rsu_r)

    cot_move.wait_recv()
    if fine:
        prepare(pre_arrived, 0)
    else:
        in_order(pre_arrived)
    rs_open(down_block, *down)

    load_wd.wait()
    piece = min(2 * LANES, hidden)

    def act_step(n, _):
        at = pl.ds(pl.multiple_of(n * piece, piece), piece)
        pa_out[:, at] = cols_dot(cg[his_f, :], wd[at, :]).astype(BF16)
        return 0
    lax.fori_loop(0, hidden // piece, act_step, 0)
    pa_move = remote(pa_out, pa_in, pa_s, pa_r, other_fs)
    pa_move.start()

    def act_own(n, _):
        at = pl.ds(pl.multiple_of(n * piece, piece), piece)
        pa_own[:, at] = cols_dot(cg[mine_f, :], wd[at, :])
        return 0
    lax.fori_loop(0, hidden // piece, act_own, 0)

    def down_step(j, _):
        prepare(pre_arrived, j)
        for d, sub in streams:
            rs_step(down_block, *down, j, d, sub)
        return 0
    lax.fori_loop(1, n_rep - 1, down_step, 0)
    prepare(pre_arrived, n_rep - 1)
    for d, sub in streams:
        rs_close(down_block, down_at, *down, agd_s, agd_r, d, sub)

    pa_move.wait_recv()

    def pre_grad(panel):
        at = lanes(panel)
        positive = jnp.maximum(pre_ref[:, at].astype(F32), 0.0)
        grad = pa_own[:, at] + pa_in[:, at].astype(F32)
        gp[mine_f, at] = (2.0 * positive * grad).astype(BF16)
        gp_copy(panel).start()
    in_order(pre_grad)
    x_move.wait_recv()
    for d, sub in streams:
        ag_step(down_at, agd_s, agd_r, 1, d, sub)
    if fine:
        prepare(gp_arrived, 0)
    else:
        in_order(gp_arrived)
    rs_open(up_block, *up)

    def both_step(j, _):
        prepare(gp_arrived, j)
        for d, sub in streams:
            ag_step(down_at, agd_s, agd_r, j + 1, d, sub)
            rs_step(up_block, *up, j, d, sub)
        return 0
    lax.fori_loop(1, n_rep - 2, both_step, 0)
    prepare(gp_arrived, n_rep - 2)
    for d, sub in streams:
        rs_step(up_block, *up, n_rep - 2, d, sub)
    prepare(gp_arrived, n_rep - 1)
    for d, sub in streams:
        ag_close(down_at, agd_s, agd_r, d, sub)
        rs_close(up_block, up_at, *up, agu_s, agu_r, d, sub)

    load_wu.wait()
    wide = min(2 * LANES, width)

    def input_out(n, _):
        at = pl.ds(pl.multiple_of(n * wide, wide), wide)
        gi_out[:, at] = cols_dot(gp[his_t, :], wu[at, :]).astype(BF16)
        return 0
    lax.fori_loop(0, width // wide, input_out, 0)
    gi_move = remote(gi_out, gi_in, gi_s, gi_r, other_tp)
    gi_move.start()

    def gather_step(j, _):
        for d, sub in streams:
            ag_step(up_at, agu_s, agu_r, j, d, sub)
        return 0
    lax.fori_loop(1, n_rep - 1, gather_step, 0)

    gi_move.wait_recv()

    def input_own(n, _):
        at = pl.ds(pl.multiple_of(n * wide, wide), wide)
        own = cols_dot(gp[mine_t, :], wu[at, :]).astype(BF16).astype(F32)
        gi_ref[:, at] = (own + gi_in[:, at].astype(F32)).astype(BF16)
        return 0
    lax.fori_loop(0, width // wide, input_own, 0)
    for d, sub in streams:
        ag_close(up_at, agu_s, agu_r, d, sub)

    for move in (cot_move, x_move, pa_move, gi_move):
        move.wait_send()

    def sent_panels(j, _):
        pre_copy(j).wait_send()
        gp_copy(j).wait_send()
        return 0
    lax.fori_loop(0, panels, sent_panels, 0)

    def sent_steps(s, _):
        for d, sub in streams:
            rs_copy(*down, d, sub, s, first_d.at[d, sub]).wait_send()
            rs_copy(*up, d, sub, s, first_u.at[d, sub]).wait_send()
            ag_copy(down_at, agd_s, agd_r, d, sub, s).wait_send()
            ag_copy(up_at, agu_s, agu_r, d, sub, s).wait_send()
        return 0
    lax.fori_loop(0, n_rep - 1, sent_steps, 0)


def scale_kernel(factor, pieces, gi, up, down, gi_out, up_out, down_out, up_wide, down_wide,
                 sems, gi_sem):
    copies = [pltpu.make_async_copy(gi, gi_out, gi_sem)]
    copies[0].start()
    for i in range(pieces):
        for n, (src, wide, dst) in enumerate(((up, up_wide, up_out), (down, down_wide, down_out))):
            rows = pl.ds(i * (src.shape[0] // pieces), src.shape[0] // pieces)
            wide[rows, :] = src[rows, :].astype(F32) * factor
            copy = pltpu.make_async_copy(wide.at[rows, :], dst.at[rows, :], sems.at[n, i])
            copy.start()
            copies.append(copy)
    for copy in copies:
        copy.wait()


def per_device(n_rep, inputs, pre_act, cotangent, up_weight, down_weight):
    half, width = inputs.shape
    hidden = pre_act.shape[1]
    panels = hidden // LANES
    subs, per_panel, w = plan(n_rep, width, hidden)
    dma = pltpu.SemaphoreType.DMA
    ring = [dma((2, subs, n_rep - 1))] * 2
    vmem = pl.BlockSpec(memory_space=pltpu.VMEM)
    anywhere = pl.BlockSpec(memory_space=pl.ANY)
    grad_inputs, grad_up, grad_down = pl.pallas_call(
        functools.partial(kernel, n_rep),
        name="ffn_backward",
        out_shape=(
            pltpu.VMEM((half, width), BF16),
            pltpu.VMEM((width, hidden), BF16),
            pltpu.VMEM((hidden, width), BF16),
        ),
        in_specs=[anywhere] * 5,
        out_specs=(vmem, vmem, vmem),
        scratch_shapes=[
            pltpu.VMEM((half, width), BF16),
            pltpu.VMEM((half, hidden), BF16),
            pltpu.VMEM((half, width), BF16),
            pltpu.VMEM((width, hidden), BF16),
            pltpu.VMEM((hidden, width), BF16),
            pltpu.VMEM((2 * half, width), BF16),
            pltpu.VMEM((2 * half, width), BF16),
            pltpu.VMEM((half, hidden), BF16),
            pltpu.VMEM((2 * half, hidden), BF16),
            pltpu.VMEM((2 * half, hidden), BF16),
            pltpu.VMEM((half, hidden), F32),
            pltpu.VMEM((half, hidden), BF16),
            pltpu.VMEM((half, hidden), BF16),
            pltpu.VMEM((half, width), BF16),
            pltpu.VMEM((half, width), BF16),
            pltpu.VMEM((2, subs, LANES, w), BF16),
            pltpu.VMEM((2, subs, w, LANES), BF16),
            pltpu.VMEM((2, subs, n_rep - 1, LANES, w), BF16),
            pltpu.VMEM((2, subs, n_rep - 1, w, LANES), BF16),
            dma((5,)), dma((2,)), dma((2,)),
            dma((panels,)), dma((panels,)), dma((panels,)), dma((panels,)),
            dma, dma, dma, dma,
            *ring, *ring, *ring, *ring,
        ],
        compiler_params=pltpu.CompilerParams(
            collective_id=0, has_side_effects=True, vmem_limit_bytes=50 * 2**20
        ),
    )(inputs, pre_act, cotangent, up_weight, down_weight)
    factor = (half * n_rep * lax.axis_size("tp")) ** (-0.5)
    pieces = 8
    return pl.pallas_call(
        functools.partial(scale_kernel, factor, pieces),
        name="scale_outputs",
        out_shape=(
            jax.ShapeDtypeStruct((half, width), BF16),
            jax.ShapeDtypeStruct((width, hidden), F32),
            jax.ShapeDtypeStruct((hidden, width), F32),
        ),
        in_specs=[vmem] * 3,
        out_specs=[anywhere] * 3,
        scratch_shapes=[
            pltpu.VMEM((width, hidden), F32),
            pltpu.VMEM((hidden, width), F32),
            dma((2, pieces)),
            dma,
        ],
        compiler_params=pltpu.CompilerParams(vmem_limit_bytes=40 * 2**20),
    )(*[pltpu.with_memory_space_constraint(g, pltpu.VMEM)
        for g in (grad_inputs, grad_up, grad_down)])


def solution(mesh):
    assert mesh.shape["fs"] == 2 and mesh.shape["tp"] == 2
    placed = (
        P(("rep", "tp"), "fs"),
        P(("rep", "fs"), "tp"),
        P(("rep", "tp"), "fs"),
        P("fs", "tp"),
        P("tp", "fs"),
    )
    return jax.shard_map(
        functools.partial(per_device, mesh.shape["rep"]),
        mesh=mesh,
        in_specs=placed,
        out_specs=(P(("rep", "tp"), "fs"), P("fs", "tp"), P("tp", "fs")),
        check_vma=False,
    )
```
